32 devices in a mesh: ep: 16 (over z, y, x), tp: 2 (over core).
Axes of the slice: x: 2, y: 2, z: 4, core: 2. Of those that a mesh axis runs over, the one named last changes fastest.
Arguments:
- tokens: bfloat16 [112, 2304], P('ep'), may hold values from -6 to 6
- attn_gain: bfloat16 [2304], replicated, may hold values from 0.099609375 to 1.8984375
- query_weight: bfloat16 [2304, 2048], P(None, 'tp'), may hold values from -0.125 to 0.125
- key_weight: bfloat16 [2304, 2048], P(None, 'tp'), may hold values from -0.125 to 0.125
- value_weight: bfloat16 [2304, 2048], P(None, 'tp'), may hold values from -0.125 to 0.125
- out_weight: bfloat16 [2304, 2048], P(None, 'tp'), may hold values from -0.125 to 0.125
- lambdas: float32 [16], P('tp'), may hold values from 0.3 to 0.8
- head_gain: bfloat16 [128], replicated, may hold values from 0.099609375 to 1.8984375
- cache_keys: bfloat16 [112, 1024, 16, 128], P('ep', None, 'tp'), may hold values from -1500 to 1500
- cache_values: bfloat16 [112, 1024, 16, 128], P('ep', None, 'tp'), may hold values from -6 to 6
- lengths: int32 [112], P('ep'), may hold values from 2 to 1024, as said below
- moe_gain: bfloat16 [2304], replicated, may hold values from 0.099609375 to 1.8984375
- gate_weight: bfloat16 [16, 2304, 1024], P('ep', None, 'tp'), may hold values from -0.125 to 0.125
- up_weight: bfloat16 [16, 2304, 1024], P('ep', None, 'tp'), may hold values from -0.125 to 0.125
- down_weight: bfloat16 [16, 1024, 2304], P('ep', 'tp'), may hold values from -0.1875 to 0.1875
- shared_gate: bfloat16 [2304, 1024], P(None, 'tp'), may hold values from -0.125 to 0.125
- shared_up: bfloat16 [2304, 1024], P(None, 'tp'), may hold values from -0.125 to 0.125
- shared_down: bfloat16 [1024, 2304], P('tp'), may hold values from -0.1875 to 0.1875
- expert_ids: int32 [112, 6], P('ep'), may hold values from 0 to 15, all different within a row; in each aligned block of 7 rows (0 to 6, 7 to 13, ...) at most 5 rows name the same one
- expert_weights: float32 [112, 6], P('ep'), may hold values from 0.2 to 1
Outputs:
- result: bfloat16 [112, 2304], P('ep', 'tp')
The draws below stay inside these ranges and needn't reach their ends.
Inputs may be any that keep to these rules, and one draw needn't show every extreme that they name: `expert_ids`: each row names 6 different experts. Among the rows of one device (aligned blocks of 7 rows) no expert is named by more than 5 rows, a bound that some block reaches. `lengths`: some sequence has 1024 cached positions.
All inputs are finite; a program needn't handle non-finite values.
Results may differ from the reference program's by a relative error of at most 0.02.
Values may be sent and summed in bfloat16 or wider, within the bound.
A program may use at most 128 MiB of HBM per device.

```python
import math
import jax
import jax.numpy as jnp
import numpy as np
from jax import lax

D = 2304
HEADS = 16
HD = 64
VD = 128
EW = 1024
SW = 1024
TOP = 6
SEQ_DEV = 7
CACHE_LEN = 1024
SEQS = 112
EXPERTS = 16
CAP = 5
N_EP = 16
N_TP = 2


def draw_cache_keys(key, part):
    base_draw = jnp.clip(jax.random.normal(key, (SEQS, CACHE_LEN, HEADS, 2 * HD), jnp.float32), -8.0, 8.0) * 1.75
    return base_draw.astype(jnp.bfloat16)


def draw_lengths(key, part):
    key_one, key_two = jax.random.split(jax.random.fold_in(key, 3))
    group_count = SEQS // SEQ_DEV
    group_top = jax.random.randint(key_one, (group_count, 1), CACHE_LEN // 4, CACHE_LEN + 1)
    drawn = jax.random.randint(key_two, (group_count, SEQ_DEV), 2, group_top + 1)
    drawn = drawn.reshape(-1).astype(jnp.int32)
    return drawn.at[0].set(CACHE_LEN)


def steps_of(rng, dims, pieces, least, high):
    def one(axis_at, blocks):
        heights = jax.random.uniform(jax.random.fold_in(jax.random.fold_in(rng, 6), axis_at), (blocks,), jnp.float32, least / len(pieces), high / len(pieces))
        return jnp.repeat(jnp.exp(heights), dims[axis_at] // blocks).reshape((-1,) + (1,) * (len(dims) - axis_at - 1))

    level = one(*pieces[0])
    for cut in pieces[1:]:
        level = level * one(*cut)
    return level


def routed_block(key, own, number, rows, count, top, bound, lean):
    order = jax.random.permutation(key, count)
    heavy_load, usual = shares(count, rows * top, bound, lean, True), shares(count, rows * top, bound, lean, False)
    places = jnp.arange(count)

    def named(tallies, offset_by):
        used = int((tallies > 0).sum())
        fixed = max(1, used // 4)
        moved = fixed + (places - fixed + offset_by * (used - fixed)) % max(1, count - fixed)
        return jnp.zeros((count,), jnp.int32).at[order[jnp.where(places < fixed, places, moved)]].set(jnp.asarray(tallies, jnp.int32))

    tallies = jnp.where(number % 4 == 0, named(heavy_load, number // 4), named(usual, number - number // 4 - 1))
    mixed = jax.random.permutation(jax.random.fold_in(own, 3), count)
    source_of, receiver = mixed[0:count // 2 * 2:2], mixed[1:count // 2 * 2:2]
    margin = jnp.minimum(tallies[source_of] - 1, bound - tallies[receiver]) // 2
    margin = jnp.where((source_of == order[0]) | (receiver == order[0]) | (tallies[receiver] == 0), 0, jnp.maximum(margin, 0))
    moved = jax.random.randint(jax.random.fold_in(own, 4), (count // 2,), 0, 1 << 20) % (margin + 1)
    tallies = tallies.at[source_of].add(-moved).at[receiver].add(moved)
    items = jnp.searchsorted(jnp.cumsum(tallies), jnp.arange(rows * top), side="right").astype(jnp.int32)
    grid = items.reshape(top, rows).T
    grid = grid[jax.random.permutation(jax.random.fold_in(own, 1), rows)]
    offset_by = jax.random.randint(jax.random.fold_in(own, 2), (rows, 1), 0, top)
    return jnp.take_along_axis(grid, (jnp.arange(top)[None, :] + offset_by) % top, axis=1)


def shares(count, total, limit, slope, full):
    portions = [(1 << 20) // math.isqrt(rank ** slope) + 1 for rank in range(1, count + 1)]
    largest = limit if full else min(limit, max(-(-total // count), total * portions[0] // sum(portions)))
    least = 1 if total - largest >= count - 1 else 0
    counts, spare = [largest] + [least] * (count - 1), total - largest - least * (count - 1)
    while spare > 0:
        candidates = [i for i in range(1, count) if counts[i] < largest] or [i for i in range(1, count) if counts[i] < limit]
        pool, remaining = sum([portions[i] for i in candidates]), spare
        for i in candidates:
            extra = min(limit - counts[i], max(1, remaining * portions[i] // pool), spare)
            counts[i] = counts[i] + extra
            spare = spare - extra
    return np.array(counts)


def bell_draw(rng, dims, width, limit, pieces=(), kind=jnp.bfloat16):
    result = width * jax.random.normal(rng, dims, jnp.float32)
    if pieces:
        result = result * steps_of(rng, dims, pieces, -0.22, 0.18)
    return jnp.clip(result, -limit, limit).astype(kind)


def setup_inputs(seed: int = 0) -> dict:
    splits = jax.random.split(jax.random.key(seed), 21)
    tokens = bell_draw(splits[0], (SEQS, D), 1.0, 6.0, ((0, 16),))
    attn_gain = jnp.clip(1.0 + 0.18 * jax.random.normal(splits[1], (D,), jnp.float32), 0.099609375, 1.8984375).astype(jnp.bfloat16)
    query_weight = bell_draw(splits[2], (D, HEADS * 2 * HD), D ** -0.5, 0.125, ((1, 2),))
    key_weight = bell_draw(splits[3], (D, HEADS * 2 * HD), D ** -0.5, 0.125, ((1, 2),))
    value_weight = bell_draw(splits[4], (D, HEADS * VD), D ** -0.5, 0.125, ((1, 2),))
    out_weight = bell_draw(splits[5], (D, HEADS * VD), (HEADS * VD) ** -0.5, 0.125, ((1, 2),))
    lambdas = jnp.clip(0.3 + 0.5 * jax.random.uniform(splits[6], (HEADS,), jnp.float32) ** steps_of(splits[6], (HEADS,), ((0, 2),), -0.2, 0.2), 0.3, 0.8)
    head_gain = jnp.clip(1.0 + 0.18 * jax.random.normal(splits[7], (VD,), jnp.float32), 0.099609375, 1.8984375).astype(jnp.bfloat16)
    cache_keys = draw_cache_keys(jax.random.fold_in(splits[20], 71), 0)
    cache_values = bell_draw(splits[9], (SEQS, CACHE_LEN, HEADS, VD), 1.0, 6.0, ((0, 16), (2, 2)))
    lengths = draw_lengths(jax.random.fold_in(splits[20], 71), 0)
    moe_gain = jnp.clip(1.0 + 0.18 * jax.random.normal(splits[11], (D,), jnp.float32), 0.099609375, 1.8984375).astype(jnp.bfloat16)
    gate_weight = bell_draw(splits[12], (EXPERTS, D, EW), D ** -0.5, 0.125, ((0, 16), (2, 2)))
    up_weight = bell_draw(splits[13], (EXPERTS, D, EW), D ** -0.5, 0.125, ((0, 16), (2, 2)))
    down_weight = bell_draw(splits[14], (EXPERTS, EW, D), EW ** -0.5, 0.1875, ((0, 16), (1, 2)))
    shared_gate = bell_draw(splits[15], (D, SW), D ** -0.5, 0.125, ((1, 2),))
    shared_up = bell_draw(splits[16], (D, SW), D ** -0.5, 0.125, ((1, 2),))
    shared_down = bell_draw(splits[17], (SW, D), SW ** -0.5, 0.1875, ((0, 2),))
    expert_ids_keys = jax.random.split(jax.random.fold_in(splits[18], 1), SEQS // SEQ_DEV)
    expert_ids_turns = jax.random.permutation(jax.random.fold_in(splits[18], 3), SEQS // SEQ_DEV)
    expert_ids = jax.vmap(lambda own, number: routed_block(jax.random.fold_in(splits[18], 2), own, number, SEQ_DEV, EXPERTS, TOP, CAP, 2))(expert_ids_keys, expert_ids_turns).reshape((SEQS, TOP))
    expert_weights = jnp.clip(0.2 + 0.8 * jax.random.uniform(splits[19], (SEQS, TOP), jnp.float32) ** steps_of(splits[19], (SEQS, TOP), ((0, 16),), -0.2, 0.2), 0.2, 1.0)
    return {"tokens": tokens, "attn_gain": attn_gain, "query_weight": query_weight, "key_weight": key_weight, "value_weight": value_weight, "out_weight": out_weight, "lambdas": lambdas, "head_gain": head_gain, "cache_keys": cache_keys, "cache_values": cache_values, "lengths": lengths, "moe_gain": moe_gain, "gate_weight": gate_weight, "up_weight": up_weight, "down_weight": down_weight, "shared_gate": shared_gate, "shared_up": shared_up, "shared_down": shared_down, "expert_ids": expert_ids, "expert_weights": expert_weights}


epsilon = 1e-06

def rms_scale(values, gain):
    wide = values.astype(jnp.float32)
    return wide * lax.rsqrt(lax.optimization_barrier(jnp.mean(wide * wide, axis=-1, keepdims=True)) + epsilon) * gain.astype(jnp.float32)

def rounded(values):
    return lax.optimization_barrier(values.astype(jnp.bfloat16)).astype(jnp.float32)

def attend_group(blocks, lambdas):
    query_rows, key_rows, value_rows, past_keys, past_values, seq_lengths = blocks
    seq_count = query_rows.shape[0]
    head_dim = past_keys.shape[-1] // 2
    score_scale = head_dim ** (-0.5)
    queries = query_rows.astype(jnp.float32).reshape(seq_count, HEADS, 2, head_dim)
    new_keys = key_rows.astype(jnp.float32).reshape(seq_count, HEADS, 2, head_dim)
    new_values = value_rows.astype(jnp.float32).reshape(seq_count, HEADS, 2 * head_dim)
    cache_rows = past_keys.astype(jnp.float32).reshape(seq_count, CACHE_LEN, HEADS, 2, head_dim)
    scores = jnp.einsum('shmd,sjhmd->shmj', queries, cache_rows) * score_scale
    own_score = lax.optimization_barrier(jnp.sum(queries * new_keys, axis=-1)) * score_scale
    live_mask = (jnp.arange(CACHE_LEN, dtype=jnp.int32)[None, :] < seq_lengths[:, None])[:, None, None, :]
    peak_score = jnp.maximum(lax.optimization_barrier(jnp.max(jnp.where(live_mask, scores, -jnp.inf), axis=-1)), own_score)
    exp_terms = jnp.where(live_mask, jnp.exp(scores - peak_score[..., None]), 0.0)
    own_term = jnp.exp(own_score - peak_score)
    denom_sum = lax.optimization_barrier(jnp.sum(exp_terms, axis=-1)) + own_term
    map_probs = exp_terms / denom_sum[..., None]
    own_prob = own_term / denom_sum
    lambda_row = lambdas[None, :]
    mixture = rounded(map_probs[:, :, 0] - lambda_row[..., None] * map_probs[:, :, 1])
    own_mixture = rounded(own_prob[:, :, 0] - lambda_row * own_prob[:, :, 1])
    head_out = jnp.einsum('shj,sjhv->shv', mixture, past_values.astype(jnp.float32))
    return head_out + own_mixture[..., None] * new_values

def reference(tokens, attn_gain, query_weight, key_weight, value_weight, out_weight, lambdas, head_gain, cache_keys, cache_values, lengths, moe_gain, gate_weight, up_weight, down_weight, shared_gate, shared_up, shared_down, expert_ids, expert_weights):
    normed = rms_scale(tokens, attn_gain).astype(jnp.bfloat16)
    query_rows = jnp.dot(normed, query_weight, preferred_element_type=jnp.float32).astype(jnp.bfloat16)
    key_new = jnp.dot(normed, key_weight, preferred_element_type=jnp.float32).astype(jnp.bfloat16)
    value_new = jnp.dot(normed, value_weight, preferred_element_type=jnp.float32).astype(jnp.bfloat16)

    def grouped(array):
        return array.reshape((N_EP, SEQ_DEV) + array.shape[1:])
    head_out = lax.map(lambda blocks: attend_group(blocks, lambdas), (grouped(query_rows), grouped(key_new), grouped(value_new), grouped(cache_keys), grouped(cache_values), grouped(lengths)))
    head_out = head_out.reshape(SEQS, HEADS, VD)
    head_normed = rms_scale(head_out, head_gain).astype(jnp.bfloat16)
    group_cols = HEADS * VD // N_TP
    head_groups = head_normed.reshape(SEQS, N_TP, group_cols).astype(jnp.float32)
    out_groups = out_weight.reshape(D, N_TP, group_cols).astype(jnp.float32)
    attn_part = rounded(jnp.einsum('snc,dnc->nsd', head_groups, out_groups))
    mixed_rows = (tokens.astype(jnp.float32) + lax.optimization_barrier(jnp.sum(attn_part, axis=0))).astype(jnp.bfloat16)
    moe_normed = rms_scale(mixed_rows, moe_gain).astype(jnp.bfloat16)
    shared_gate_out = jnp.dot(moe_normed, shared_gate, preferred_element_type=jnp.float32)
    shared_up_out = jnp.dot(moe_normed, shared_up, preferred_element_type=jnp.float32)
    shared_hidden = (jax.nn.silu(shared_gate_out) * shared_up_out).astype(jnp.bfloat16)
    shared_cols = SW // N_TP
    shared_part = rounded(jnp.einsum('snc,ncd->nsd', shared_hidden.reshape(SEQS, N_TP, shared_cols).astype(jnp.float32), shared_down.reshape(N_TP, shared_cols, D).astype(jnp.float32)))
    shared_out = lax.optimization_barrier(jnp.sum(shared_part, axis=0))
    slot_ids = expert_ids.reshape(N_EP, SEQ_DEV * TOP).astype(jnp.int32)
    expert_hits = (slot_ids[..., None] == jnp.arange(EXPERTS, dtype=jnp.int32)[None, None, :]).astype(jnp.int32)
    earlier = jnp.cumsum(expert_hits, axis=1).astype(jnp.int32) - expert_hits
    slot_rank = lax.optimization_barrier(jnp.sum(earlier * expert_hits, axis=-1)).astype(jnp.int32)
    slot_row = (jnp.arange(N_EP, dtype=jnp.int32)[:, None] * CAP + slot_rank).reshape(-1)
    slot_token = (jnp.arange(SEQS * TOP, dtype=jnp.int32) // TOP).astype(jnp.int32)
    flat_ids = slot_ids.reshape(-1)
    expert_rows = jnp.zeros((EXPERTS, N_EP * CAP, D), jnp.bfloat16)
    expert_rows = expert_rows.at[flat_ids, slot_row].set(moe_normed[slot_token])
    expert_cols = EW // N_TP

    def run_expert(blocks):
        row_block, gate_block, up_block, down_block = blocks
        gate_out = jnp.dot(row_block, gate_block, preferred_element_type=jnp.float32)
        up_out = jnp.dot(row_block, up_block, preferred_element_type=jnp.float32)
        expert_hidden = (jax.nn.silu(gate_out) * up_out).astype(jnp.bfloat16)
        partials = jnp.einsum('rnc,ncd->nrd', expert_hidden.reshape(N_EP * CAP, N_TP, expert_cols).astype(jnp.float32), down_block.reshape(N_TP, expert_cols, D).astype(jnp.float32))
        return lax.optimization_barrier(jnp.sum(rounded(partials), axis=0)).astype(jnp.bfloat16)
    expert_out = lax.map(run_expert, (expert_rows, gate_weight, up_weight, down_weight))
    slot_values = expert_out[flat_ids, slot_row].astype(jnp.float32).reshape(SEQS, TOP, D)
    routed = lax.optimization_barrier(jnp.sum(expert_weights[:, :, None] * slot_values, axis=1))
    return (mixed_rows.astype(jnp.float32) + routed + shared_out).astype(jnp.bfloat16)
```

```python
import functools
import jax
import jax.numpy as jnp
from jax import lax
from jax.experimental import pallas as pl
from jax.experimental.pallas import tpu as pltpu
from jax.sharding import PartitionSpec as P

epsilon = 1e-06


def rms_scale(values, gain):
    wide = values.astype(jnp.float32)
    return (
        wide
        * lax.rsqrt(jnp.mean(wide * wide, axis=-1, keepdims=True) + epsilon)
        * gain.astype(jnp.float32)
    )


def plain_shards(
    tokens,
    attn_gain,
    query_weight,
    key_weight,
    value_weight,
    out_weight,
    lambdas,
    head_gain,
    cache_keys,
    cache_values,
    lengths,
    moe_gain,
    gate_weight,
    up_weight,
    down_weight,
    shared_gate,
    shared_up,
    shared_down,
    expert_ids,
    expert_weights,
):
    seq_dev, model_width = tokens.shape
    local_heads = lambdas.shape[0]
    head_dim = cache_keys.shape[-1] // 2
    cache_len = cache_keys.shape[1]
    normed = rms_scale(tokens, attn_gain).astype(jnp.bfloat16)
    query_rows = jnp.dot(normed, query_weight, preferred_element_type=jnp.float32).astype(
        jnp.bfloat16
    )
    key_new = jnp.dot(normed, key_weight, preferred_element_type=jnp.float32).astype(jnp.bfloat16)
    value_new = jnp.dot(normed, value_weight, preferred_element_type=jnp.float32).astype(
        jnp.bfloat16
    )
    score_scale = head_dim ** (-0.5)
    queries = query_rows.reshape(seq_dev, local_heads, 2, head_dim)
    new_keys = key_new.reshape(seq_dev, local_heads, 2, head_dim)
    new_values = value_new.reshape(seq_dev, local_heads, 2 * head_dim)
    past_keys = cache_keys.reshape(seq_dev, cache_len, local_heads, 2, head_dim)
    scores = (
        jnp.einsum("shmd,sjhmd->shmj", queries, past_keys, preferred_element_type=jnp.float32)
        * score_scale
    )
    own_score = (
        jnp.sum(queries.astype(jnp.float32) * new_keys.astype(jnp.float32), axis=-1) * score_scale
    )
    live_mask = (jnp.arange(cache_len, dtype=jnp.int32)[None, :] < lengths[:, None])[
        :, None, None, :
    ]
    peak_score = jnp.maximum(jnp.max(jnp.where(live_mask, scores, -jnp.inf), axis=-1), own_score)
    exp_terms = jnp.where(live_mask, jnp.exp(scores - peak_score[..., None]), 0.0)
    own_term = jnp.exp(own_score - peak_score)
    denom_sum = jnp.sum(exp_terms, axis=-1) + own_term
    map_probs = exp_terms / denom_sum[..., None]
    own_prob = own_term / denom_sum
    lambda_row = lambdas[None, :]
    mixture = (map_probs[:, :, 0] - lambda_row[..., None] * map_probs[:, :, 1]).astype(jnp.bfloat16)
    own_mixture = (own_prob[:, :, 0] - lambda_row * own_prob[:, :, 1]).astype(jnp.bfloat16)
    head_out = jnp.einsum(
        "shj,sjhv->shv", mixture, cache_values, preferred_element_type=jnp.float32
    )
    head_out = head_out + own_mixture.astype(jnp.float32)[..., None] * new_values.astype(
        jnp.float32
    )
    head_normed = (
        rms_scale(head_out, head_gain)
        .astype(jnp.bfloat16)
        .reshape(seq_dev, local_heads * 2 * head_dim)
    )
    attn_part = lax.dot_general(
        head_normed, out_weight, (((1,), (1,)), ((), ())), preferred_element_type=jnp.float32
    )
    attn_total = lax.psum(attn_part.astype(jnp.bfloat16), "tp").astype(jnp.float32)
    mixed_rows = (tokens.astype(jnp.float32) + attn_total).astype(jnp.bfloat16)
    moe_normed = rms_scale(mixed_rows, moe_gain).astype(jnp.bfloat16)
    shared_gate_out = jnp.dot(moe_normed, shared_gate, preferred_element_type=jnp.float32)
    shared_up_out = jnp.dot(moe_normed, shared_up, preferred_element_type=jnp.float32)
    shared_hidden = (jax.nn.silu(shared_gate_out) * shared_up_out).astype(jnp.bfloat16)
    shared_part = jnp.dot(shared_hidden, shared_down, preferred_element_type=jnp.float32)
    experts = lax.axis_size("ep")
    top_count = expert_ids.shape[1]
    capacity = min(seq_dev, max(2, 2 * seq_dev * top_count // experts))
    slot_count = seq_dev * top_count
    slot_ids = expert_ids.reshape(slot_count)
    expert_hits = (slot_ids[:, None] == jnp.arange(experts, dtype=jnp.int32)[None, :]).astype(
        jnp.int32
    )
    slot_rank = jnp.sum((jnp.cumsum(expert_hits, axis=0) - expert_hits) * expert_hits, axis=1)
    slot_place = slot_ids * capacity + slot_rank
    placed = (
        slot_place[:, None] == jnp.arange(experts * capacity, dtype=jnp.int32)[None, :]
    ).astype(jnp.bfloat16)
    slot_token = jnp.arange(slot_count, dtype=jnp.int32) // top_count
    token_pick = (slot_token[:, None] == jnp.arange(seq_dev, dtype=jnp.int32)[None, :]).astype(
        jnp.bfloat16
    )
    dispatch = lax.dot_general(
        placed, token_pick, (((0,), (0,)), ((), ())), preferred_element_type=jnp.float32
    ).astype(jnp.bfloat16)
    col_count = model_width // lax.axis_size("tp")
    own_start = lax.axis_index("tp") * col_count
    own_normed = lax.dynamic_slice_in_dim(moe_normed, own_start, col_count, 1)
    send_slice = jnp.dot(dispatch, own_normed, preferred_element_type=jnp.float32).astype(
        jnp.bfloat16
    )
    arrived = lax.all_to_all(send_slice, "ep", split_axis=0, concat_axis=0, tiled=True)
    received = lax.all_gather(arrived, "tp", axis=1, tiled=True)
    gate_out = jnp.dot(received, gate_weight[0], preferred_element_type=jnp.float32)
    up_out = jnp.dot(received, up_weight[0], preferred_element_type=jnp.float32)
    expert_hidden = (jax.nn.silu(gate_out) * up_out).astype(jnp.bfloat16)
    expert_part = jnp.dot(expert_hidden, down_weight[0], preferred_element_type=jnp.float32)
    expert_sum, shared_out = (
        lax.psum_scatter(
            expert_part.astype(jnp.bfloat16), "tp", scatter_dimension=1, tiled=True
        ).astype(jnp.float32),
        lax.psum_scatter(
            shared_part.astype(jnp.bfloat16), "tp", scatter_dimension=1, tiled=True
        ).astype(jnp.float32),
    )
    returned = lax.all_to_all(
        expert_sum.astype(jnp.bfloat16), "ep", split_axis=0, concat_axis=0, tiled=True
    )
    slot_values = jnp.dot(placed, returned, preferred_element_type=jnp.float32).reshape(
        seq_dev, top_count, col_count
    )
    routed = jnp.sum(expert_weights[:, :, None] * slot_values, axis=1)
    own_cols = lax.dynamic_slice_in_dim(mixed_rows, own_start, col_count, 1)
    return (own_cols.astype(jnp.float32) + routed + shared_out).astype(jnp.bfloat16)


BLOCK = 256
PIECES = 4
MESH = pl.DeviceIdType.MESH
NT = (((1,), (1,)), ((), ()))


def attend_kernel(
    lengths_ref, tokens_ref, gain_ref, lambdas_ref, head_gain_ref,
    wq_hbm, wk_hbm, wv_hbm, wo_hbm, keys_hbm, values_hbm,
    out_ref,
    wq, wk, wv, wo, keys, values, q_rows, k_rows, v_rows, head_rows,
    w_sem, key_sem, value_sem,
):
    seqs, width = tokens_ref.shape
    heads = lambdas_ref.shape[0]
    head_dim = 64
    block_rows = BLOCK * heads
    depth = width // PIECES

    def weight_copy(index, piece):
        source = (wq_hbm, wk_hbm, wv_hbm, wo_hbm)[index]
        target = (wq, wk, wv, wo)[index]
        rows = pl.ds(piece * depth, depth)
        return pltpu.make_async_copy(source.at[rows], target.at[rows], w_sem.at[index, piece])

    def key_copy(s, b):
        rows = pl.ds(b * block_rows, block_rows)
        return pltpu.make_async_copy(keys_hbm.at[s, rows], keys.at[s, rows], key_sem.at[s, b])

    def value_copy(s, b):
        rows = pl.ds(b * block_rows, block_rows)
        return pltpu.make_async_copy(values_hbm.at[s, rows], values.at[s, rows], value_sem.at[s, b])

    def block_count(s):
        return (lengths_ref[s] + (BLOCK - 1)) // BLOCK

    def start_cache(s):
        @pl.loop(0, block_count(s))
        def _(b):
            key_copy(s, b).start()
            value_copy(s, b).start()

    for index in range(3):
        for piece in range(PIECES):
            weight_copy(index, piece).start()

    @pl.loop(0, seqs - 1)
    def _(s):
        start_cache(s)

    for piece in range(PIECES):
        weight_copy(3, piece).start()
    start_cache(seqs - 1)

    normed = rms_scale(tokens_ref[...], gain_ref[...]).astype(jnp.bfloat16)
    for index, (weight, rows_ref) in enumerate(((wq, q_rows), (wk, k_rows), (wv, v_rows))):
        total = None
        for piece in range(PIECES):
            weight_copy(index, piece).wait()
            rows = slice(piece * depth, (piece + 1) * depth)
            term = jnp.dot(normed[:, rows], weight[rows, :], preferred_element_type=jnp.float32)
            total = term if total is None else total + term
        total = total.astype(jnp.bfloat16).astype(jnp.float32)
        for h in range(heads):
            rows_ref[0:seqs, h, :] = total[:, h * 128 : (h + 1) * 128]

    scale = head_dim ** (-0.5)
    lane = lax.broadcasted_iota(jnp.int32, (heads, 128), 1)
    col = lax.broadcasted_iota(jnp.int32, (2 * heads, block_rows), 1)
    row = lax.broadcasted_iota(jnp.int32, (2 * heads, block_rows), 0)
    own_head = lax.rem(col, heads) == lax.rem(row, heads)
    col = jnp.where(own_head, col, jnp.int32(1 << 30))
    lam = lambdas_ref[...]
    head_rows[...] = jnp.zeros_like(head_rows)

    @pl.loop(0, seqs)
    def _(s):
        query = q_rows[s]
        pair = jnp.concatenate(
            [jnp.where(lane < head_dim, query, 0.0), jnp.where(lane < head_dim, 0.0, query)], axis=0
        )
        new_key = k_rows[s]
        new_value = v_rows[s]
        peak = (
            jnp.sum(pair * jnp.concatenate([new_key, new_key], axis=0), axis=1, keepdims=True)
            * scale
        )
        denom = jnp.ones_like(peak)
        total = jnp.concatenate([new_value, new_value], axis=0)
        query_pair = pair.astype(jnp.bfloat16)

        def step(b, state):
            peak, denom, total = state
            key_copy(s, b).wait()
            rows = pl.ds(pl.multiple_of(b * block_rows, block_rows), block_rows)
            scores = (
                lax.dot_general(query_pair, keys[s, rows], NT, preferred_element_type=jnp.float32)
                * scale
            )
            live = col < (lengths_ref[s] - b * BLOCK) * heads
            scores = jnp.where(live, scores, -jnp.inf)
            new_peak = jnp.maximum(peak, jnp.max(scores, axis=1, keepdims=True))
            fade = jnp.exp(peak - new_peak)
            terms = jnp.exp(scores - new_peak)
            value_copy(s, b).wait()
            denom = denom * fade + jnp.sum(terms, axis=1, keepdims=True)
            total = total * fade + jnp.dot(
                terms.astype(jnp.bfloat16), values[s, rows], preferred_element_type=jnp.float32
            )
            return new_peak, denom, total

        peak, denom, total = lax.fori_loop(0, block_count(s), step, (peak, denom, total))
        probs = total / denom
        head_out = probs[0:heads] - lam * probs[heads:]
        head_rows[:, s, :] = rms_scale(head_out, head_gain_ref[...])

    flat = jnp.concatenate([head_rows[h] for h in range(heads)], axis=1).astype(jnp.bfloat16)
    for piece in range(PIECES):
        weight_copy(3, piece).wait()
        rows = slice(piece * depth, (piece + 1) * depth)
        out_ref[:, rows] = lax.dot_general(
            flat, wo[rows, :], NT, preferred_element_type=jnp.float32
        ).astype(jnp.bfloat16)


def attend(tokens, gain, wq, wk, wv, wo, lambdas, head_gain, cache_keys, cache_values, lengths):
    seqs, width = tokens.shape
    heads = lambdas.shape[0]
    cache_len = cache_keys.shape[1]
    blocks = cache_len // BLOCK
    flat = (seqs, cache_len * heads, 128)
    vmem = pl.BlockSpec(memory_space=pltpu.VMEM)
    hbm = pl.BlockSpec(memory_space=pl.ANY)
    return pl.pallas_call(
        attend_kernel,
        out_shape=jax.ShapeDtypeStruct((8, width), jnp.bfloat16),
        in_specs=[pl.BlockSpec(memory_space=pltpu.SMEM)] + [vmem] * 4 + [hbm] * 6,
        out_specs=vmem,
        scratch_shapes=[pltpu.VMEM(wq.shape, jnp.bfloat16)] * 4
        + [pltpu.VMEM(flat, jnp.bfloat16)] * 2
        + [pltpu.VMEM((8, heads, 128), jnp.float32)] * 3
        + [pltpu.VMEM((heads, 8, 128), jnp.float32)]
        + [
            pltpu.SemaphoreType.DMA((4, PIECES)),
            pltpu.SemaphoreType.DMA((seqs, blocks)),
            pltpu.SemaphoreType.DMA((seqs, blocks)),
        ],
        compiler_params=pltpu.CompilerParams(vmem_limit_bytes=60 << 20),
        name="attend",
    )(
        lengths, tokens, gain.reshape(1, width), lambdas.reshape(heads, 1),
        head_gain.reshape(1, 128), wq, wk, wv, wo,
        cache_keys.reshape(flat), cache_values.reshape(flat),
    )


def experts_kernel(
    count,
    part_ref, tokens_ref, gain_ref, ids_ref, weights_ref,
    gate_hbm, up_hbm, down_hbm, sgate_hbm, sup_hbm, sdown_hbm,
    out_ref,
    gate, up, down, sgate, sup, sdown,
    part_in, mixed, normed, send, arrived, other, give_sum, take_sum, back, returned,
    give_shared, take_shared,
    w_sem, pair_send, pair_recv, go_send, go_recv, fill_send, fill_recv, ret_send, ret_recv,
):
    seqs, width = tokens_ref.shape
    slots = send.shape[1]
    cols = width // 2
    me = lax.axis_index("ep")
    half = lax.axis_index("tp")
    peer = (me, 1 - half)
    rows_all = count * slots
    my_cols = pl.ds(pl.multiple_of(half * cols, 128), cols)
    peer_cols = pl.ds(pl.multiple_of((1 - half) * cols, 128), cols)

    loads = [
        pltpu.make_async_copy(source, target, w_sem.at[i])
        for i, (source, target) in enumerate(
            (
                (sgate_hbm, sgate), (sup_hbm, sup), (sdown_hbm, sdown),
                (gate_hbm.at[0], gate), (up_hbm.at[0], up), (down_hbm.at[0], down),
            )
        )
    ]
    for load in loads:
        load.start()

    barrier = pltpu.get_barrier_semaphore()
    pl.semaphore_signal(barrier, inc=1, device_id=peer, device_id_type=MESH)
    for i in range(1, count):
        pl.semaphore_signal(
            barrier, inc=1, device_id=(lax.rem(me + i, count), half), device_id_type=MESH
        )
    mixed[...] = jnp.zeros_like(mixed)
    c_expert = lax.broadcasted_iota(jnp.int32, (seqs, rows_all), 1) // slots
    c_rank = lax.rem(lax.broadcasted_iota(jnp.int32, (seqs, rows_all), 1), slots)
    hits = jnp.zeros((seqs, rows_all), jnp.float32)
    gains = jnp.zeros((seqs, rows_all), jnp.float32)
    for k in range(ids_ref.shape[1]):
        same = (ids_ref[:, k : k + 1] == c_expert).astype(jnp.float32)
        hits = hits + same
        gains = gains + same * weights_ref[:, k : k + 1]
    ranks = [jnp.zeros((1, rows_all), jnp.float32)]
    for t in range(1, seqs):
        ranks.append(ranks[-1] + hits[t - 1 : t])
    rank = jnp.concatenate(ranks, axis=0)
    placed = jnp.where(rank == c_rank.astype(jnp.float32), hits, 0.0)
    gains = gains * placed
    pad = jnp.zeros((8 - seqs, rows_all), jnp.float32)
    spread = jnp.concatenate([placed, pad], axis=0).T.astype(jnp.bfloat16)

    def pair_copy(source, target, i):
        return pltpu.make_async_remote_copy(
            src_ref=source, dst_ref=target, send_sem=pair_send.at[i], recv_sem=pair_recv.at[i],
            device_id=peer, device_id_type=MESH,
        )

    pl.semaphore_wait(barrier, count)
    part_copy = pair_copy(part_ref, part_in, 0)
    part_copy.start()
    part_copy.wait()
    attn = part_ref[...].astype(jnp.float32) + part_in[...].astype(jnp.float32)
    mixed[0:seqs, :] = (
        (tokens_ref[...].astype(jnp.float32) + attn[0:seqs]).astype(jnp.bfloat16).astype(jnp.float32)
    )
    row = rms_scale(mixed[...], gain_ref[...]).astype(jnp.bfloat16)
    normed[...] = row
    outgoing = jnp.dot(spread, normed[:, my_cols], preferred_element_type=jnp.float32)
    for e in range(count):
        send[e] = outgoing[e * slots : (e + 1) * slots].astype(jnp.bfloat16)

    def go_copy(i):
        to = lax.rem(me + i, count)
        return pltpu.make_async_remote_copy(
            src_ref=send.at[to], dst_ref=arrived.at[me], send_sem=go_send.at[i],
            recv_sem=go_recv.at[i], device_id=(to, half), device_id_type=MESH,
        )

    for i in range(1, count):
        go_copy(i).start()
    arrived[me] = send[me]

    for load in loads[:3]:
        load.wait()
    shared_g = jnp.dot(row, sgate[...], preferred_element_type=jnp.float32)
    shared_u = jnp.dot(row, sup[...], preferred_element_type=jnp.float32)
    shared_h = (jax.nn.silu(shared_g) * shared_u).astype(jnp.bfloat16)
    give_shared[...] = jnp.dot(
        shared_h, sdown[:, peer_cols], preferred_element_type=jnp.float32
    ).astype(jnp.bfloat16)
    shared_copy = pair_copy(give_shared, take_shared, 1)
    shared_copy.start()
    shared_own = jnp.dot(shared_h, sdown[:, my_cols], preferred_element_type=jnp.float32)
    shared_own = shared_own.astype(jnp.bfloat16).astype(jnp.float32)

    def fill_copy(i):
        source = lax.rem(me - i + count, count)
        return pltpu.make_async_remote_copy(
            src_ref=arrived.at[source], dst_ref=other.at[source], send_sem=fill_send.at[i],
            recv_sem=fill_recv.at[i], device_id=peer, device_id_type=MESH,
        )

    fill_copy(0).start()
    for i in range(1, count):
        go_copy(i).wait()
        fill_copy(i).start()
    for load in loads[3:5]:
        load.wait()
    mine = arrived[...].astype(jnp.float32).reshape(rows_all, cols).astype(jnp.bfloat16)
    my_rows = pl.ds(pl.multiple_of(half * cols, 128), cols)
    peer_rows = pl.ds(pl.multiple_of((1 - half) * cols, 128), cols)
    gate_out = jnp.dot(mine, gate[my_rows, :], preferred_element_type=jnp.float32)
    up_out = jnp.dot(mine, up[my_rows, :], preferred_element_type=jnp.float32)
    for i in range(count):
        fill_copy(i).wait()
    theirs = other[...].astype(jnp.float32).reshape(rows_all, cols).astype(jnp.bfloat16)
    gate_out = gate_out + jnp.dot(theirs, gate[peer_rows, :], preferred_element_type=jnp.float32)
    up_out = up_out + jnp.dot(theirs, up[peer_rows, :], preferred_element_type=jnp.float32)
    hidden = (jax.nn.silu(gate_out) * up_out).astype(jnp.bfloat16)
    loads[5].wait()
    give_sum[...] = jnp.dot(
        hidden, down[:, peer_cols], preferred_element_type=jnp.float32
    ).astype(jnp.bfloat16)
    sum_copy = pair_copy(give_sum, take_sum, 2)
    sum_copy.start()
    own_sum = jnp.dot(hidden, down[:, my_cols], preferred_element_type=jnp.float32)
    own_sum = own_sum.astype(jnp.bfloat16).astype(jnp.float32)
    sum_copy.wait()
    total = own_sum + take_sum[...].astype(jnp.float32)
    for e in range(count):
        back[e] = total[e * slots : (e + 1) * slots].astype(jnp.bfloat16)

    def ret_copy(i):
        to = lax.rem(me + i, count)
        return pltpu.make_async_remote_copy(
            src_ref=back.at[to], dst_ref=returned.at[me], send_sem=ret_send.at[i],
            recv_sem=ret_recv.at[i], device_id=(to, half), device_id_type=MESH,
        )

    for i in range(1, count):
        ret_copy(i).start()
    returned[me] = back[me]
    shared_copy.wait()
    result = mixed[:, my_cols] + (shared_own + take_shared[...].astype(jnp.float32))
    high = gains.astype(jnp.bfloat16)
    low = (gains - high.astype(jnp.float32)).astype(jnp.bfloat16)
    for i in range(1, count):
        ret_copy(i).wait()
    values = returned[...].astype(jnp.float32).reshape(rows_all, cols).astype(jnp.bfloat16)
    routed = jnp.dot(high, values, preferred_element_type=jnp.float32) + jnp.dot(
        low, values, preferred_element_type=jnp.float32
    )
    out_ref[...] = (result[0:seqs] + routed).astype(jnp.bfloat16)


def run_experts(
    count, part, tokens, gain, ids, weights, gate, up, down, sgate, sup, sdown
):
    seqs, width = tokens.shape
    capacity = min(seqs, max(2, 2 * seqs * ids.shape[1] // count))
    slots = -(-capacity // 8) * 8
    cols = width // 2
    vmem = pl.BlockSpec(memory_space=pltpu.VMEM)
    hbm = pl.BlockSpec(memory_space=pl.ANY)
    half_rows = pltpu.VMEM((count, slots, cols), jnp.bfloat16)
    flat_rows = pltpu.VMEM((count * slots, cols), jnp.bfloat16)
    each = pltpu.SemaphoreType.DMA((count,))
    return pl.pallas_call(
        functools.partial(experts_kernel, count),
        out_shape=jax.ShapeDtypeStruct((seqs, cols), jnp.bfloat16),
        in_specs=[vmem] * 5 + [hbm] * 6,
        out_specs=vmem,
        scratch_shapes=[
            pltpu.VMEM(w.shape[-2:], jnp.bfloat16) for w in (gate, up, down, sgate, sup, sdown)
        ]
        + [
            pltpu.VMEM((8, width), jnp.bfloat16),
            pltpu.VMEM((8, width), jnp.float32),
            pltpu.VMEM((8, width), jnp.bfloat16),
            half_rows, half_rows, half_rows, flat_rows, flat_rows, half_rows, half_rows,
            pltpu.VMEM((8, cols), jnp.bfloat16),
            pltpu.VMEM((8, cols), jnp.bfloat16),
            pltpu.SemaphoreType.DMA((6,)),
            pltpu.SemaphoreType.DMA((3,)),
            pltpu.SemaphoreType.DMA((3,)),
            each, each, each, each, each, each,
        ],
        compiler_params=pltpu.CompilerParams(
            collective_id=0, has_side_effects=True, vmem_limit_bytes=40 << 20
        ),
        name="experts",
    )(part, tokens, gain.reshape(1, width), ids, weights, gate, up, down, sgate, sup, sdown)


def fast_shards(
    tokens, attn_gain, query_weight, key_weight, value_weight, out_weight, lambdas, head_gain,
    cache_keys, cache_values, lengths, moe_gain, gate_weight, up_weight, down_weight,
    shared_gate, shared_up, shared_down, expert_ids, expert_weights,
):
    part = attend(
        tokens, attn_gain, query_weight, key_weight, value_weight, out_weight, lambdas, head_gain,
        cache_keys, cache_values, lengths,
    )
    return run_experts(
        lax.axis_size("ep"), part, tokens, moe_gain, expert_ids, expert_weights,
        gate_weight, up_weight, down_weight, shared_gate, shared_up, shared_down,
    )


def pick_shards(mesh):
    return fast_shards if mesh.shape["tp"] == 2 else plain_shards


def solution(mesh):
    in_specs = (
        P("ep", None),
        P(),
        P(None, "tp"),
        P(None, "tp"),
        P(None, "tp"),
        P(None, "tp"),
        P("tp"),
        P(),
        P("ep", None, "tp", None),
        P("ep", None, "tp", None),
        P("ep"),
        P(),
        P("ep", None, "tp"),
        P("ep", None, "tp"),
        P("ep", "tp", None),
        P(None, "tp"),
        P(None, "tp"),
        P("tp", None),
        P("ep", None),
        P("ep", None),
    )
    out_specs = P("ep", "tp")
    return jax.shard_map(pick_shards(mesh), mesh=mesh, in_specs=in_specs, out_specs=out_specs, check_vma=False)
```

```python
import functools
import jax
import jax.numpy as jnp
from jax import lax
from jax.experimental import pallas as pl
from jax.experimental.pallas import tpu as pltpu
from jax.sharding import PartitionSpec as P

epsilon = 1e-06


def rms_scale(values, gain):
    wide = values.astype(jnp.float32)
    return (
        wide
        * lax.rsqrt(jnp.mean(wide * wide, axis=-1, keepdims=True) + epsilon)
        * gain.astype(jnp.float32)
    )


def plain_shards(
    tokens,
    attn_gain,
    query_weight,
    key_weight,
    value_weight,
    out_weight,
    lambdas,
    head_gain,
    cache_keys,
    cache_values,
    lengths,
    moe_gain,
    gate_weight,
    up_weight,
    down_weight,
    shared_gate,
    shared_up,
    shared_down,
    expert_ids,
    expert_weights,
):
    seq_dev, model_width = tokens.shape
    local_heads = lambdas.shape[0]
    head_dim = cache_keys.shape[-1] // 2
    cache_len = cache_keys.shape[1]
    normed = rms_scale(tokens, attn_gain).astype(jnp.bfloat16)
    query_rows = jnp.dot(normed, query_weight, preferred_element_type=jnp.float32).astype(
        jnp.bfloat16
    )
    key_new = jnp.dot(normed, key_weight, preferred_element_type=jnp.float32).astype(jnp.bfloat16)
    value_new = jnp.dot(normed, value_weight, preferred_element_type=jnp.float32).astype(
        jnp.bfloat16
    )
    score_scale = head_dim ** (-0.5)
    queries = query_rows.reshape(seq_dev, local_heads, 2, head_dim)
    new_keys = key_new.reshape(seq_dev, local_heads, 2, head_dim)
    new_values = value_new.reshape(seq_dev, local_heads, 2 * head_dim)
    past_keys = cache_keys.reshape(seq_dev, cache_len, local_heads, 2, head_dim)
    scores = (
        jnp.einsum("shmd,sjhmd->shmj", queries, past_keys, preferred_element_type=jnp.float32)
        * score_scale
    )
    own_score = (
        jnp.sum(queries.astype(jnp.float32) * new_keys.astype(jnp.float32), axis=-1) * score_scale
    )
    live_mask = (jnp.arange(cache_len, dtype=jnp.int32)[None, :] < lengths[:, None])[
        :, None, None, :
    ]
    peak_score = jnp.maximum(jnp.max(jnp.where(live_mask, scores, -jnp.inf), axis=-1), own_score)
    exp_terms = jnp.where(live_mask, jnp.exp(scores - peak_score[..., None]), 0.0)
    own_term = jnp.exp(own_score - peak_score)
    denom_sum = jnp.sum(exp_terms, axis=-1) + own_term
    map_probs = exp_terms / denom_sum[..., None]
    own_prob = own_term / denom_sum
    lambda_row = lambdas[None, :]
    mixture = (map_probs[:, :, 0] - lambda_row[..., None] * map_probs[:, :, 1]).astype(jnp.bfloat16)
    own_mixture = (own_prob[:, :, 0] - lambda_row * own_prob[:, :, 1]).astype(jnp.bfloat16)
    head_out = jnp.einsum(
        "shj,sjhv->shv", mixture, cache_values, preferred_element_type=jnp.float32
    )
    head_out = head_out + own_mixture.astype(jnp.float32)[..., None] * new_values.astype(
        jnp.float32
    )
    head_normed = (
        rms_scale(head_out, head_gain)
        .astype(jnp.bfloat16)
        .reshape(seq_dev, local_heads * 2 * head_dim)
    )
    attn_part = lax.dot_general(
        head_normed, out_weight, (((1,), (1,)), ((), ())), preferred_element_type=jnp.float32
    )
    attn_total = lax.psum(attn_part.astype(jnp.bfloat16), "tp").astype(jnp.float32)
    mixed_rows = (tokens.astype(jnp.float32) + attn_total).astype(jnp.bfloat16)
    moe_normed = rms_scale(mixed_rows, moe_gain).astype(jnp.bfloat16)
    shared_gate_out = jnp.dot(moe_normed, shared_gate, preferred_element_type=jnp.float32)
    shared_up_out = jnp.dot(moe_normed, shared_up, preferred_element_type=jnp.float32)
    shared_hidden = (jax.nn.silu(shared_gate_out) * shared_up_out).astype(jnp.bfloat16)
    shared_part = jnp.dot(shared_hidden, shared_down, preferred_element_type=jnp.float32)
    experts = lax.axis_size("ep")
    top_count = expert_ids.shape[1]
    capacity = min(seq_dev, max(2, 2 * seq_dev * top_count // experts))
    slot_count = seq_dev * top_count
    slot_ids = expert_ids.reshape(slot_count)
    expert_hits = (slot_ids[:, None] == jnp.arange(experts, dtype=jnp.int32)[None, :]).astype(
        jnp.int32
    )
    slot_rank = jnp.sum((jnp.cumsum(expert_hits, axis=0) - expert_hits) * expert_hits, axis=1)
    slot_place = slot_ids * capacity + slot_rank
    placed = (
        slot_place[:, None] == jnp.arange(experts * capacity, dtype=jnp.int32)[None, :]
    ).astype(jnp.bfloat16)
    slot_token = jnp.arange(slot_count, dtype=jnp.int32) // top_count
    token_pick = (slot_token[:, None] == jnp.arange(seq_dev, dtype=jnp.int32)[None, :]).astype(
        jnp.bfloat16
    )
    dispatch = lax.dot_general(
        placed, token_pick, (((0,), (0,)), ((), ())), preferred_element_type=jnp.float32
    ).astype(jnp.bfloat16)
    col_count = model_width // lax.axis_size("tp")
    own_start = lax.axis_index("tp") * col_count
    own_normed = lax.dynamic_slice_in_dim(moe_normed, own_start, col_count, 1)
    send_slice = jnp.dot(dispatch, own_normed, preferred_element_type=jnp.float32).astype(
        jnp.bfloat16
    )
    arrived = lax.all_to_all(send_slice, "ep", split_axis=0, concat_axis=0, tiled=True)
    received = lax.all_gather(arrived, "tp", axis=1, tiled=True)
    gate_out = jnp.dot(received, gate_weight[0], preferred_element_type=jnp.float32)
    up_out = jnp.dot(received, up_weight[0], preferred_element_type=jnp.float32)
    expert_hidden = (jax.nn.silu(gate_out) * up_out).astype(jnp.bfloat16)
    expert_part = jnp.dot(expert_hidden, down_weight[0], preferred_element_type=jnp.float32)
    expert_sum, shared_out = (
        lax.psum_scatter(
            expert_part.astype(jnp.bfloat16), "tp", scatter_dimension=1, tiled=True
        ).astype(jnp.float32),
        lax.psum_scatter(
            shared_part.astype(jnp.bfloat16), "tp", scatter_dimension=1, tiled=True
        ).astype(jnp.float32),
    )
    returned = lax.all_to_all(
        expert_sum.astype(jnp.bfloat16), "ep", split_axis=0, concat_axis=0, tiled=True
    )
    slot_values = jnp.dot(placed, returned, preferred_element_type=jnp.float32).reshape(
        seq_dev, top_count, col_count
    )
    routed = jnp.sum(expert_weights[:, :, None] * slot_values, axis=1)
    own_cols = lax.dynamic_slice_in_dim(mixed_rows, own_start, col_count, 1)
    return (own_cols.astype(jnp.float32) + routed + shared_out).astype(jnp.bfloat16)


BLOCK = 256
PIECES = 4
MESH = pl.DeviceIdType.MESH
NT = (((1,), (1,)), ((), ()))


def attend_kernel(
    lengths_ref, tokens_ref, gain_ref, lambdas_ref, head_gain_ref,
    wq_hbm, wk_hbm, wv_hbm, wo_hbm, keys_hbm, values_hbm,
    out_ref,
    wq, wk, wv, wo, keys, values, q_rows, k_rows, v_rows, head_rows,
    w_sem, key_sem, value_sem,
):
    seqs, width = tokens_ref.shape
    heads = lambdas_ref.shape[0]
    head_dim = 64
    block_rows = BLOCK * heads
    depth = width // PIECES

    def weight_copy(index, piece):
        source = (wq_hbm, wk_hbm, wv_hbm, wo_hbm)[index]
        target = (wq, wk, wv, wo)[index]
        rows = pl.ds(piece * depth, depth)
        return pltpu.make_async_copy(source.at[rows], target.at[rows], w_sem.at[index, piece])

    def key_copy(s, b):
        rows = pl.ds(b * block_rows, block_rows)
        return pltpu.make_async_copy(keys_hbm.at[s, rows], keys.at[s, rows], key_sem.at[s, b])

    def value_copy(s, b):
        rows = pl.ds(b * block_rows, block_rows)
        return pltpu.make_async_copy(values_hbm.at[s, rows], values.at[s, rows], value_sem.at[s, b])

    def block_count(s):
        return (lengths_ref[s] + (BLOCK - 1)) // BLOCK

    def start_cache(s):
        @pl.loop(0, block_count(s))
        def _(b):
            key_copy(s, b).start()
            value_copy(s, b).start()

    for index in range(3):
        for piece in range(PIECES):
            weight_copy(index, piece).start()

    @pl.loop(0, seqs - 1)
    def _(s):
        start_cache(s)

    for piece in range(PIECES):
        weight_copy(3, piece).start()
    start_cache(seqs - 1)

    normed = rms_scale(tokens_ref[...], gain_ref[...].astype(jnp.float32).reshape(1, width)).astype(jnp.bfloat16)
    for index, (weight, rows_ref) in enumerate(((wq, q_rows), (wk, k_rows), (wv, v_rows))):
        total = None
        for piece in range(PIECES):
            weight_copy(index, piece).wait()
            rows = slice(piece * depth, (piece + 1) * depth)
            term = jnp.dot(normed[:, rows], weight[rows, :], preferred_element_type=jnp.float32)
            total = term if total is None else total + term
        total = total.astype(jnp.bfloat16).astype(jnp.float32)
        for h in range(heads):
            rows_ref[0:seqs, h, :] = total[:, h * 128 : (h + 1) * 128]

    scale = head_dim ** (-0.5)
    lane = lax.broadcasted_iota(jnp.int32, (heads, 128), 1)
    col = lax.broadcasted_iota(jnp.int32, (2 * heads, block_rows), 1)
    row = lax.broadcasted_iota(jnp.int32, (2 * heads, block_rows), 0)
    own_head = lax.rem(col, heads) == lax.rem(row, heads)
    col = jnp.where(own_head, col, jnp.int32(1 << 30))
    head_at = lax.broadcasted_iota(jnp.int32, (heads, 1), 0)
    lam = jnp.zeros((heads, 1), jnp.float32)
    for h in range(heads):
        lam = jnp.where(head_at == h, lambdas_ref[h], lam)
    head_rows[...] = jnp.zeros_like(head_rows)

    @pl.loop(0, seqs)
    def _(s):
        query = q_rows[s]
        pair = jnp.concatenate(
            [jnp.where(lane < head_dim, query, 0.0), jnp.where(lane < head_dim, 0.0, query)], axis=0
        )
        new_key = k_rows[s]
        new_value = v_rows[s]
        peak = (
            jnp.sum(pair * jnp.concatenate([new_key, new_key], axis=0), axis=1, keepdims=True)
            * scale
        )
        denom = jnp.ones_like(peak)
        total = jnp.concatenate([new_value, new_value], axis=0)
        query_pair = pair.astype(jnp.bfloat16)

        def step(b, state):
            peak, denom, total = state
            key_copy(s, b).wait()
            rows = pl.ds(pl.multiple_of(b * block_rows, block_rows), block_rows)
            scores = (
                lax.dot_general(query_pair, keys[s, rows], NT, preferred_element_type=jnp.float32)
                * scale
            )
            live = col < (lengths_ref[s] - b * BLOCK) * heads
            scores = jnp.where(live, scores, -jnp.inf)
            new_peak = jnp.maximum(peak, jnp.max(scores, axis=1, keepdims=True))
            fade = jnp.exp(peak - new_peak)
            terms = jnp.exp(scores - new_peak)
            value_copy(s, b).wait()
            denom = denom * fade + jnp.sum(terms, axis=1, keepdims=True)
            total = total * fade + jnp.dot(
                terms.astype(jnp.bfloat16), values[s, rows], preferred_element_type=jnp.float32
            )
            return new_peak, denom, total

        peak, denom, total = lax.fori_loop(0, block_count(s), step, (peak, denom, total))
        probs = total / denom
        head_out = probs[0:heads] - lam * probs[heads:]
        head_rows[:, s, :] = rms_scale(head_out, head_gain_ref[...])

    flat = jnp.concatenate([head_rows[h] for h in range(heads)], axis=1).astype(jnp.bfloat16)
    for piece in range(PIECES):
        weight_copy(3, piece).wait()
        rows = slice(piece * depth, (piece + 1) * depth)
        out_ref[:, rows] = lax.dot_general(
            flat, wo[rows, :], NT, preferred_element_type=jnp.float32
        ).astype(jnp.bfloat16)


def attend(tokens, gain, wq, wk, wv, wo, lambdas, head_gain, cache_keys, cache_values, lengths):
    seqs, width = tokens.shape
    heads = lambdas.shape[0]
    cache_len = cache_keys.shape[1]
    blocks = cache_len // BLOCK
    flat = (seqs, cache_len * heads, 128)
    vmem = pl.BlockSpec(memory_space=pltpu.VMEM)
    smem = pl.BlockSpec(memory_space=pltpu.SMEM)
    hbm = pl.BlockSpec(memory_space=pltpu.HBM)
    return pl.pallas_call(
        attend_kernel,
        out_shape=jax.ShapeDtypeStruct((8, width), jnp.bfloat16),
        in_specs=[smem, vmem, vmem, smem, vmem] + [hbm] * 6,
        out_specs=vmem,
        scratch_shapes=[pltpu.VMEM(wq.shape, jnp.bfloat16)] * 4
        + [pltpu.VMEM(flat, jnp.bfloat16)] * 2
        + [pltpu.VMEM((8, heads, 128), jnp.float32)] * 3
        + [pltpu.VMEM((heads, 8, 128), jnp.float32)]
        + [
            pltpu.SemaphoreType.DMA((4, PIECES)),
            pltpu.SemaphoreType.DMA((seqs, blocks)),
            pltpu.SemaphoreType.DMA((seqs, blocks)),
        ],
        compiler_params=pltpu.CompilerParams(vmem_limit_bytes=60 << 20),
        name="attend",
    )(
        lengths, tokens, gain, lambdas,
        head_gain.reshape(1, 128), wq, wk, wv, wo,
        cache_keys.reshape(flat), cache_values.reshape(flat),
    )


def experts_kernel(
    count,
    part_ref, tokens_ref, gain_ref, ids_ref, weights_ref,
    gate_hbm, up_hbm, down_hbm, sgate_hbm, sup_hbm, sdown_hbm,
    out_ref,
    gate, up, down, sgate, sup, sdown,
    part_in, mixed, normed, send, arrived, other, give_sum, take_sum, back, returned,
    give_shared, take_shared,
    w_sem, pair_send, pair_recv, go_send, go_recv, fill_send, fill_recv, ret_send, ret_recv,
):
    seqs, width = tokens_ref.shape
    slots = send.shape[1]
    cols = width // 2
    me = lax.axis_index("ep")
    half = lax.axis_index("tp")
    peer = (me, 1 - half)
    rows_all = count * slots
    my_cols = pl.ds(pl.multiple_of(half * cols, 128), cols)
    peer_cols = pl.ds(pl.multiple_of((1 - half) * cols, 128), cols)

    loads = [
        pltpu.make_async_copy(source, target, w_sem.at[i])
        for i, (source, target) in enumerate(
            (
                (sgate_hbm, sgate), (sup_hbm, sup), (sdown_hbm, sdown),
                (gate_hbm.at[0], gate), (up_hbm.at[0], up), (down_hbm.at[0], down),
            )
        )
    ]
    for load in loads:
        load.start()

    barrier = pltpu.get_barrier_semaphore()
    pl.semaphore_signal(barrier, inc=1, device_id=peer, device_id_type=MESH)
    for i in range(1, count):
        pl.semaphore_signal(
            barrier, inc=1, device_id=(lax.rem(me + i, count), half), device_id_type=MESH
        )
    mixed[...] = jnp.zeros_like(mixed)
    c_expert = lax.broadcasted_iota(jnp.int32, (seqs, rows_all), 1) // slots
    c_rank = lax.rem(lax.broadcasted_iota(jnp.int32, (seqs, rows_all), 1), slots)
    hits = jnp.zeros((seqs, rows_all), jnp.float32)
    gains = jnp.zeros((seqs, rows_all), jnp.float32)
    for k in range(ids_ref.shape[1]):
        same = (ids_ref[:, k : k + 1] == c_expert).astype(jnp.float32)
        hits = hits + same
        gains = gains + same * weights_ref[:, k : k + 1]
    ranks = [jnp.zeros((1, rows_all), jnp.float32)]
    for t in range(1, seqs):
        ranks.append(ranks[-1] + hits[t - 1 : t])
    rank = jnp.concatenate(ranks, axis=0)
    placed = jnp.where(rank == c_rank.astype(jnp.float32), hits, 0.0)
    gains = gains * placed
    pad = jnp.zeros((8 - seqs, rows_all), jnp.float32)
    spread = jnp.concatenate([placed, pad], axis=0).T.astype(jnp.bfloat16)

    def pair_copy(source, target, i):
        return pltpu.make_async_remote_copy(
            src_ref=source, dst_ref=target, send_sem=pair_send.at[i], recv_sem=pair_recv.at[i],
            device_id=peer, device_id_type=MESH,
        )

    pl.semaphore_wait(barrier, count)
    part_copy = pair_copy(part_ref, part_in, 0)
    part_copy.start()
    part_copy.wait()
    attn = part_ref[...].astype(jnp.float32) + part_in[...].astype(jnp.float32)
    mixed[0:seqs, :] = (
        (tokens_ref[...].astype(jnp.float32) + attn[0:seqs]).astype(jnp.bfloat16).astype(jnp.float32)
    )
    row = rms_scale(mixed[...], gain_ref[...].astype(jnp.float32).reshape(1, width)).astype(jnp.bfloat16)
    normed[...] = row
    outgoing = jnp.dot(spread, normed[:, my_cols], preferred_element_type=jnp.float32)
    for e in range(count):
        send[e] = outgoing[e * slots : (e + 1) * slots].astype(jnp.bfloat16)

    def go_copy(i):
        to = lax.rem(me + i, count)
        return pltpu.make_async_remote_copy(
            src_ref=send.at[to], dst_ref=arrived.at[me], send_sem=go_send.at[i],
            recv_sem=go_recv.at[i], device_id=(to, half), device_id_type=MESH,
        )

    for i in range(1, count):
        go_copy(i).start()
    arrived[me] = send[me]

    for load in loads[:3]:
        load.wait()
    shared_g = jnp.dot(row, sgate[...], preferred_element_type=jnp.float32)
    shared_u = jnp.dot(row, sup[...], preferred_element_type=jnp.float32)
    shared_h = (jax.nn.silu(shared_g) * shared_u).astype(jnp.bfloat16)
    give_shared[...] = jnp.dot(
        shared_h, sdown[:, peer_cols], preferred_element_type=jnp.float32
    ).astype(jnp.bfloat16)
    shared_copy = pair_copy(give_shared, take_shared, 1)
    shared_copy.start()
    shared_own = jnp.dot(shared_h, sdown[:, my_cols], preferred_element_type=jnp.float32)
    shared_own = shared_own.astype(jnp.bfloat16).astype(jnp.float32)

    def fill_copy(i):
        source = lax.rem(me - i + count, count)
        return pltpu.make_async_remote_copy(
            src_ref=arrived.at[source], dst_ref=other.at[source], send_sem=fill_send.at[i],
            recv_sem=fill_recv.at[i], device_id=peer, device_id_type=MESH,
        )

    fill_copy(0).start()
    for i in range(1, count):
        go_copy(i).wait()
        fill_copy(i).start()
    for load in loads[3:5]:
        load.wait()
    mine = arrived[...].astype(jnp.float32).reshape(rows_all, cols).astype(jnp.bfloat16)
    my_rows = pl.ds(pl.multiple_of(half * cols, 128), cols)
    peer_rows = pl.ds(pl.multiple_of((1 - half) * cols, 128), cols)
    gate_out = jnp.dot(mine, gate[my_rows, :], preferred_element_type=jnp.float32)
    up_out = jnp.dot(mine, up[my_rows, :], preferred_element_type=jnp.float32)
    for i in range(count):
        fill_copy(i).wait()
    theirs = other[...].astype(jnp.float32).reshape(rows_all, cols).astype(jnp.bfloat16)
    gate_out = gate_out + jnp.dot(theirs, gate[peer_rows, :], preferred_element_type=jnp.float32)
    up_out = up_out + jnp.dot(theirs, up[peer_rows, :], preferred_element_type=jnp.float32)
    hidden = (jax.nn.silu(gate_out) * up_out).astype(jnp.bfloat16)
    loads[5].wait()
    give_sum[...] = jnp.dot(
        hidden, down[:, peer_cols], preferred_element_type=jnp.float32
    ).astype(jnp.bfloat16)
    sum_copy = pair_copy(give_sum, take_sum, 2)
    sum_copy.start()
    own_sum = jnp.dot(hidden, down[:, my_cols], preferred_element_type=jnp.float32)
    own_sum = own_sum.astype(jnp.bfloat16).astype(jnp.float32)
    sum_copy.wait()
    total = own_sum + take_sum[...].astype(jnp.float32)
    for e in range(count):
        back[e] = total[e * slots : (e + 1) * slots].astype(jnp.bfloat16)

    def ret_copy(i):
        to = lax.rem(me + i, count)
        return pltpu.make_async_remote_copy(
            src_ref=back.at[to], dst_ref=returned.at[me], send_sem=ret_send.at[i],
            recv_sem=ret_recv.at[i], device_id=(to, half), device_id_type=MESH,
        )

    for i in range(1, count):
        ret_copy(i).start()
    returned[me] = back[me]
    shared_copy.wait()
    result = mixed[:, my_cols] + (shared_own + take_shared[...].astype(jnp.float32))
    high = gains.astype(jnp.bfloat16)
    low = (gains - high.astype(jnp.float32)).astype(jnp.bfloat16)
    for i in range(1, count):
        ret_copy(i).wait()
    values = returned[...].astype(jnp.float32).reshape(rows_all, cols).astype(jnp.bfloat16)
    routed = jnp.dot(high, values, preferred_element_type=jnp.float32) + jnp.dot(
        low, values, preferred_element_type=jnp.float32
    )
    out_ref[...] = (result[0:seqs] + routed).astype(jnp.bfloat16)


def run_experts(
    count, part, tokens, gain, ids, weights, gate, up, down, sgate, sup, sdown
):
    seqs, width = tokens.shape
    capacity = min(seqs, max(2, 2 * seqs * ids.shape[1] // count))
    slots = -(-capacity // 8) * 8
    cols = width // 2
    vmem = pl.BlockSpec(memory_space=pltpu.VMEM)
    hbm = pl.BlockSpec(memory_space=pltpu.HBM)
    half_rows = pltpu.VMEM((count, slots, cols), jnp.bfloat16)
    flat_rows = pltpu.VMEM((count * slots, cols), jnp.bfloat16)
    each = pltpu.SemaphoreType.DMA((count,))
    return pl.pallas_call(
        functools.partial(experts_kernel, count),
        out_shape=jax.ShapeDtypeStruct((seqs, cols), jnp.bfloat16),
        in_specs=[vmem] * 5 + [hbm] * 6,
        out_specs=vmem,
        scratch_shapes=[
            pltpu.VMEM(w.shape[-2:], jnp.bfloat16) for w in (gate, up, down, sgate, sup, sdown)
        ]
        + [
            pltpu.VMEM((8, width), jnp.bfloat16),
            pltpu.VMEM((8, width), jnp.float32),
            pltpu.VMEM((8, width), jnp.bfloat16),
            half_rows, half_rows, half_rows, flat_rows, flat_rows, half_rows, half_rows,
            pltpu.VMEM((8, cols), jnp.bfloat16),
            pltpu.VMEM((8, cols), jnp.bfloat16),
            pltpu.SemaphoreType.DMA((6,)),
            pltpu.SemaphoreType.DMA((3,)),
            pltpu.SemaphoreType.DMA((3,)),
            each, each, each, each, each, each,
        ],
        compiler_params=pltpu.CompilerParams(
            collective_id=0, has_side_effects=True, vmem_limit_bytes=60 << 20
        ),
        name="experts",
    )(part, tokens, gain, ids, weights, gate, up, down, sgate, sup, sdown)


def fast_shards(
    tokens, attn_gain, query_weight, key_weight, value_weight, out_weight, lambdas, head_gain,
    cache_keys, cache_values, lengths, moe_gain, gate_weight, up_weight, down_weight,
    shared_gate, shared_up, shared_down, expert_ids, expert_weights,
):
    part = attend(
        tokens, attn_gain, query_weight, key_weight, value_weight, out_weight, lambdas, head_gain,
        cache_keys, cache_values, lengths,
    )
    return run_experts(
        lax.axis_size("ep"), part, tokens, moe_gain, expert_ids, expert_weights,
        gate_weight, up_weight, down_weight, shared_gate, shared_up, shared_down,
    )


def pick_shards(mesh):
    return fast_shards if mesh.shape["tp"] == 2 else plain_shards


def solution(mesh):
    in_specs = (
        P("ep", None),
        P(),
        P(None, "tp"),
        P(None, "tp"),
        P(None, "tp"),
        P(None, "tp"),
        P("tp"),
        P(),
        P("ep", None, "tp", None),
        P("ep", None, "tp", None),
        P("ep"),
        P(),
        P("ep", None, "tp"),
        P("ep", None, "tp"),
        P("ep", "tp", None),
        P(None, "tp"),
        P(None, "tp"),
        P("tp", None),
        P("ep", None),
        P("ep", None),
    )
    out_specs = P("ep", "tp")
    return jax.shard_map(pick_shards(mesh), mesh=mesh, in_specs=in_specs, out_specs=out_specs, check_vma=False)
```
